32 devices in a mesh: grp: 2 (over y), sp: 4 (over z), tp: 4 (over x, core).
Axes of the slice: x: 2, y: 2, z: 4, core: 2. Of those that a mesh axis runs over, the one named last changes fastest.
Arguments:
- latent: bfloat16 [2048, 512], P(('grp', 'sp')), parts along dimension 0, may hold values from -6 to 6
- rope_key: bfloat16 [2048, 64], P(('grp', 'sp')), parts along dimension 0, may hold values from -6 to 6
- wide_query: bfloat16 [2048, 1536], P(('grp', 'sp'), 'tp'), parts along dimension 0, may hold values from -1300 to 1300
- narrow_query: bfloat16 [2048, 1024], P(('grp', 'sp'), 'tp'), parts along dimension 0, may hold values from -1300 to 1300
- wide_key_weight: bfloat16 [512, 1024], P(None, 'tp'), may hold values from -0.25 to 0.25
- wide_value_weight: bfloat16 [512, 1024], P(None, 'tp'), may hold values from -0.25 to 0.25
- narrow_key_weight: bfloat16 [512, 512], P(None, 'tp'), may hold values from -0.25 to 0.25
- narrow_value_weight: bfloat16 [512, 512], P(None, 'tp'), may hold values from -0.25 to 0.25
- latent_norm_scale: float32 [512], replicated, may hold values from 0.1 to 1.9
- out_wide: bfloat16 [1024, 4096], P('tp'), may hold values from -0.4375 to 0.4375
- out_narrow: bfloat16 [512, 4096], P('tp'), may hold values from -0.4375 to 0.4375
- residual: bfloat16 [2048, 4096], P(('grp', 'sp', 'tp')), parts along dimension 0, may hold values from -6 to 6
- ffn_gain: float32 [4096], replicated, may hold values from 0.1 to 1.9
- shared_gate: bfloat16 [4096, 512], P(None, 'tp'), may hold values from -0.09375 to 0.09375
- shared_up: bfloat16 [4096, 512], P(None, 'tp'), may hold values from -0.09375 to 0.09375
- shared_down: bfloat16 [512, 4096], P('tp'), may hold values from -0.25 to 0.25
- expert_gate: bfloat16 [16, 4096, 192], P(('sp', 'tp')), may hold values from -0.09375 to 0.09375
- expert_up: bfloat16 [16, 4096, 192], P(('sp', 'tp')), may hold values from -0.09375 to 0.09375
- expert_down: bfloat16 [16, 192, 4096], P(('sp', 'tp')), may hold values from -0.4375 to 0.4375
- routes: int32 [2048, 2], P(('grp', 'sp', 'tp')), parts along dimension 0, may hold values from 0 to 15, all different within a row; in each aligned block of 64 rows (0 to 63, 64 to 127, ...) at most 16 rows name the same one
- route_weights: float32 [2048, 2], P(('grp', 'sp', 'tp')), parts along dimension 0, may hold values from 0.25 to 1.5
Outputs:
- layer_out: bfloat16 [2048, 4096], P(('grp', 'sp', 'tp')), parts along dimension 0
The draws below stay inside these ranges and needn't reach their ends.
There are 2 independent parts, one for each index of `grp`. The reference program is written for one: setup_inputs(seed, part) draws one part's arguments, and reference() takes and returns one part's arrays. A program takes and returns all parts, laid end to end along the dimension named above; an argument that names none is the same for every part. Nothing has to cross between parts.
Inputs may be any that keep to these rules, and one draw needn't show every extreme that they name: `routes`: each row names 2 different experts; in each aligned block of 64 rows no expert is named by more than 16 rows, and some block has an expert named exactly 16 times.
All inputs are finite; a program needn't handle non-finite values.
Results may differ from the reference program's by a relative error of at most 0.023.
Values may be sent and summed in bfloat16 or wider, within the bound.
A program may use at most 128 MiB of HBM per device.

```python
import math
import jax
import jax.numpy as jnp
import numpy as np
from jax import lax

D = 4096
LATENT_WIDTH = 512
ROPE = 64
FIRST_HEADS = 8
WIDE_HEAD_SIZE = 128
SECOND_HEADS = 8
NARROW_HEAD_SIZE = 64
SHARED_FF = 512
EXPERT_FF = 192
TOPK = 2
TOKEN_COUNT = 1024
ROWS = 64
EXPERTS = 16
CAP = 16
N_SP = 4
N_TP = 4


def query_values(key, columns):
    values = jnp.clip(2.5 * jax.random.normal(key, (TOKEN_COUNT, columns), jnp.float32), -15.0, 15.0)
    return values.astype(jnp.bfloat16)


def draw_wide_query(key, part):
    return query_values(jax.random.fold_in(key, 11), FIRST_HEADS * (WIDE_HEAD_SIZE + ROPE))


def draw_narrow_query(key, part):
    return query_values(jax.random.fold_in(key, 23), SECOND_HEADS * (NARROW_HEAD_SIZE + ROPE))


def levels(own_key, shape, cuts, low, largest):
    level = 1.0
    for dim, blocks in cuts:
        heights = jax.random.uniform(jax.random.fold_in(jax.random.fold_in(own_key, 6), dim), (blocks,), jnp.float32, low / len(cuts), largest / len(cuts))
        level = level * jnp.repeat(jnp.exp(heights), shape[dim] // blocks).reshape((-1,) + (1,) * (len(shape) - 1 - dim))
    return level


def deal_out(stream_key, own, number, rows, count, top, limit, skew):
    order = jax.random.permutation(stream_key, count)
    crowded, ordinary = portions_of(count, rows * top, limit, skew, True), portions_of(count, rows * top, limit, skew, False)
    places = jnp.arange(count)

    def named(lengths, turn):
        used = int((lengths > 0).sum())
        fixed = max(1, used // 4)
        passed = fixed + (places - fixed + turn * (used - fixed)) % max(1, count - fixed)
        return jnp.zeros((count,), jnp.int32).at[order[jnp.where(places < fixed, places, passed)]].set(jnp.asarray(lengths, jnp.int32))

    lengths = jnp.where(number % 4 == 0, named(crowded, number // 4), named(ordinary, number - number // 4 - 1))
    mixed = jax.random.permutation(jax.random.fold_in(own, 3), count)
    source_of, receiver = mixed[0:count // 2 * 2:2], mixed[1:count // 2 * 2:2]
    slack = jnp.minimum(lengths[source_of] - 1, limit - lengths[receiver]) // 2
    slack = jnp.where((source_of == order[0]) | (receiver == order[0]) | (lengths[receiver] == 0), 0, jnp.maximum(slack, 0))
    passed = jax.random.randint(jax.random.fold_in(own, 4), (count // 2,), 0, 1 << 20) % (slack + 1)
    lengths = lengths.at[source_of].add(-passed).at[receiver].add(passed)
    items = jnp.searchsorted(jnp.cumsum(lengths), jnp.arange(rows * top), side="right").astype(jnp.int32)
    grid = items.reshape(top, rows).T
    grid = grid[jax.random.permutation(jax.random.fold_in(own, 1), rows)]
    turn = jax.random.randint(jax.random.fold_in(own, 2), (rows, 1), 0, top)
    return jnp.take_along_axis(grid, (jnp.arange(top)[None, :] + turn) % top, axis=1)


def portions_of(number_of, total, reach, slope, full):
    weights = [(1 << 20) // math.isqrt(standing ** slope) + 1 for standing in range(1, number_of + 1)]
    largest = reach if full else min(reach, max(-(-total // number_of), total * weights[0] // sum(weights)))
    least = 1 if total - largest >= number_of - 1 else 0
    counts, surplus = [largest] + [least] * (number_of - 1), total - largest - least * (number_of - 1)
    while surplus > 0:
        free = [i for i in range(1, number_of) if counts[i] < largest] or [i for i in range(1, number_of) if counts[i] < reach]
        whole, budget = sum([weights[i] for i in free]), surplus
        for i in free:
            addition = min(reach - counts[i], max(1, budget * weights[i] // whole), surplus)
            counts[i] = counts[i] + addition
            surplus = surplus - addition
    return np.array(counts)


def centred(stream_key, extent, width, bound, shards=(), kind=jnp.bfloat16):
    level = levels(stream_key, extent, shards, -0.22, 0.18) if shards else 1.0
    drawn = jax.random.normal(stream_key, extent, jnp.float32) * width * level
    return jnp.minimum(jnp.maximum(drawn, -bound), bound).astype(kind)


def setup_inputs(seed: int = 0, part: int = 0) -> dict:
    key_list = jax.random.split(jax.random.key(seed), 22)
    part_splits = jax.random.split(jax.random.fold_in(key_list[21], part), 22)
    latent = centred(part_splits[0], (TOKEN_COUNT, LATENT_WIDTH), 1.0, 6.0, ((0, 4),))
    rope_key = centred(part_splits[1], (TOKEN_COUNT, ROPE), 1.0, 6.0, ((0, 4),))
    wide_query = draw_wide_query(jax.random.fold_in(jax.random.fold_in(key_list[21], part), 71), part)
    narrow_query = draw_narrow_query(jax.random.fold_in(jax.random.fold_in(key_list[21], part), 71), part)
    wide_key_weight = centred(key_list[4], (LATENT_WIDTH, FIRST_HEADS * WIDE_HEAD_SIZE), LATENT_WIDTH ** -0.5, 0.25, ((1, 4),))
    wide_value_weight = centred(key_list[5], (LATENT_WIDTH, FIRST_HEADS * WIDE_HEAD_SIZE), LATENT_WIDTH ** -0.5, 0.25, ((1, 4),))
    narrow_key_weight = centred(key_list[6], (LATENT_WIDTH, SECOND_HEADS * NARROW_HEAD_SIZE), LATENT_WIDTH ** -0.5, 0.25, ((1, 4),))
    narrow_value_weight = centred(key_list[7], (LATENT_WIDTH, SECOND_HEADS * NARROW_HEAD_SIZE), LATENT_WIDTH ** -0.5, 0.25, ((1, 4),))
    latent_norm_scale = jnp.clip(1.0 + 0.18 * jax.random.normal(key_list[8], (LATENT_WIDTH,), jnp.float32), 0.1, 1.9)
    out_wide = centred(key_list[9], (FIRST_HEADS * WIDE_HEAD_SIZE, D), ((FIRST_HEADS * WIDE_HEAD_SIZE + SECOND_HEADS * NARROW_HEAD_SIZE) // 8) ** -0.5, 0.4375, ((0, 4),))
    out_narrow = centred(key_list[10], (SECOND_HEADS * NARROW_HEAD_SIZE, D), ((FIRST_HEADS * WIDE_HEAD_SIZE + SECOND_HEADS * NARROW_HEAD_SIZE) // 8) ** -0.5, 0.4375, ((0, 4),))
    residual = centred(part_splits[11], (TOKEN_COUNT, D), 1.0, 6.0, ((0, 16),))
    ffn_gain = jnp.clip(1.0 + 0.18 * jax.random.normal(key_list[12], (D,), jnp.float32), 0.1, 1.9)
    shared_gate = centred(key_list[13], (D, SHARED_FF), D ** -0.5, 0.09375, ((1, 4),))
    shared_up = centred(key_list[14], (D, SHARED_FF), D ** -0.5, 0.09375, ((1, 4),))
    shared_down = centred(key_list[15], (SHARED_FF, D), SHARED_FF ** -0.5, 0.25, ((0, 4),))
    expert_gate = centred(key_list[16], (EXPERTS, D, EXPERT_FF), D ** -0.5, 0.09375, ((0, 16),))
    expert_up = centred(key_list[17], (EXPERTS, D, EXPERT_FF), D ** -0.5, 0.09375, ((0, 16),))
    expert_down = centred(key_list[18], (EXPERTS, EXPERT_FF, D), EXPERT_FF ** -0.5, 0.4375, ((0, 16),))
    routes_keys = jax.random.split(jax.random.fold_in(part_splits[19], 1), TOKEN_COUNT // ROWS)
    routes_turns = jax.random.permutation(jax.random.fold_in(part_splits[19], 3), TOKEN_COUNT // ROWS)
    routes = jax.vmap(lambda own, number: deal_out(jax.random.fold_in(part_splits[19], 2), own, number, ROWS, EXPERTS, TOPK, CAP, 1))(routes_keys, routes_turns).reshape((TOKEN_COUNT, TOPK))
    route_weights = jnp.clip(0.25 + 1.25 * jax.random.uniform(part_splits[20], (TOKEN_COUNT, TOPK), jnp.float32) ** levels(part_splits[20], (TOKEN_COUNT, TOPK), ((0, 16),), -0.2, 0.2), 0.25, 1.5)
    return {"latent": latent, "rope_key": rope_key, "wide_query": wide_query, "narrow_query": narrow_query, "wide_key_weight": wide_key_weight, "wide_value_weight": wide_value_weight, "narrow_key_weight": narrow_key_weight, "narrow_value_weight": narrow_value_weight, "latent_norm_scale": latent_norm_scale, "out_wide": out_wide, "out_narrow": out_narrow, "residual": residual, "ffn_gain": ffn_gain, "shared_gate": shared_gate, "shared_up": shared_up, "shared_down": shared_down, "expert_gate": expert_gate, "expert_up": expert_up, "expert_down": expert_down, "routes": routes, "route_weights": route_weights}


EPS = 1e-06
ROPE_BASE = 10000.0
NEG_FILL = -1e+30

def rounded(values):
    return lax.optimization_barrier(values.astype(jnp.bfloat16)).astype(jnp.float32)

def rotate(values, positions):
    half_size = values.shape[-1] // 2
    inverse = ROPE_BASE ** (-jnp.arange(half_size, dtype=jnp.float32) * 2.0 / values.shape[-1])
    angles = positions.astype(jnp.float32)[:, None] * inverse[None, :]
    shaped = (angles.shape[0],) + (1,) * (values.ndim - 2) + (half_size,)
    cosine_table = jnp.cos(angles).reshape(shaped)
    sine_table = jnp.sin(angles).reshape(shaped)
    first_half = values[..., :half_size]
    second_half = values[..., half_size:]
    return jnp.concatenate([first_half * cosine_table - second_half * sine_table, second_half * cosine_table + first_half * sine_table], axis=-1)

def rms_scale(values, gain):
    return values * lax.rsqrt(lax.optimization_barrier(jnp.mean(values * values, axis=-1, keepdims=True)) + EPS) * gain

def update(state, query_plain, query_turned, keys, turned_rows, values, visible, factor):
    running_max, running_sum, weighted = state
    scores = jnp.einsum('qhd,khd->hqk', query_plain.astype(jnp.float32), keys.astype(jnp.float32))
    scores = scores + jnp.einsum('qhr,kr->hqk', query_turned.astype(jnp.float32), turned_rows.astype(jnp.float32))
    scores = jnp.where(visible[None], scores * factor, NEG_FILL)
    new_max = jnp.maximum(running_max, lax.optimization_barrier(jnp.max(scores, axis=2)))
    probs = jnp.where(visible[None], jnp.exp(scores - new_max[:, :, None]), 0.0)
    fading = jnp.exp(running_max - new_max)
    running_sum = running_sum * fading + lax.optimization_barrier(jnp.sum(probs, axis=2))
    weighted = weighted * fading[:, :, None] + jnp.einsum('hqk,khd->hqd', rounded(probs), values.astype(jnp.float32))
    return (new_max, running_sum, weighted)

def attend_group(query_plain, query_turned, keys, values, turned_keys, factor):
    tokens_all, heads, value_size = values.shape
    block = math.gcd(tokens_all, 512)
    blocks_all = tokens_all // block

    def per_query(block_index):
        query_start = block_index * block
        plain_rows = lax.dynamic_slice_in_dim(query_plain, query_start, block, 0)
        turned_rows_q = lax.dynamic_slice_in_dim(query_turned, query_start, block, 0)
        query_pos = query_start + jnp.arange(block, dtype=jnp.int32)

        def per_key(key_index, state):
            key_start = key_index * block
            key_pos = key_start + jnp.arange(block, dtype=jnp.int32)
            visible = key_pos[None, :] <= query_pos[:, None]
            return update(state, plain_rows, turned_rows_q, lax.dynamic_slice_in_dim(keys, key_start, block, 0), lax.dynamic_slice_in_dim(turned_keys, key_start, block, 0), lax.dynamic_slice_in_dim(values, key_start, block, 0), visible, factor)
        initial = (jnp.full((heads, block), NEG_FILL, jnp.float32), jnp.zeros((heads, block), jnp.float32), jnp.zeros((heads, block, value_size), jnp.float32))
        final = lax.fori_loop(0, block_index + 1, per_key, initial)
        normal_sampler = final[2] / final[1][:, :, None]
        return normal_sampler.astype(jnp.bfloat16).transpose(1, 0, 2).reshape(block, heads * value_size)
    outputs = lax.map(per_query, jnp.arange(blocks_all, dtype=jnp.int32))
    return outputs.reshape(tokens_all, heads * value_size)

def reference(latent, rope_key, wide_query, narrow_query, wide_key_weight, wide_value_weight, narrow_key_weight, narrow_value_weight, latent_norm_scale, out_wide, out_narrow, residual, ffn_gain, shared_gate, shared_up, shared_down, expert_gate, expert_up, expert_down, routes, route_weights):
    positions = jnp.arange(TOKEN_COUNT, dtype=jnp.int32)
    normed_latent = rms_scale(latent.astype(jnp.float32), latent_norm_scale).astype(jnp.bfloat16)
    turned_key = rotate(rope_key.astype(jnp.float32), positions).astype(jnp.bfloat16)
    wide_heads_q = wide_query.reshape(TOKEN_COUNT, FIRST_HEADS, WIDE_HEAD_SIZE + ROPE)
    wide_plain = wide_heads_q[..., :WIDE_HEAD_SIZE]
    wide_turned = rotate(wide_heads_q[..., WIDE_HEAD_SIZE:].astype(jnp.float32), positions).astype(jnp.bfloat16)
    narrow_heads_q = narrow_query.reshape(TOKEN_COUNT, SECOND_HEADS, NARROW_HEAD_SIZE + ROPE)
    narrow_plain = narrow_heads_q[..., :NARROW_HEAD_SIZE]
    narrow_turned = rotate(narrow_heads_q[..., NARROW_HEAD_SIZE:].astype(jnp.float32), positions).astype(jnp.bfloat16)
    wide_keys = jnp.dot(normed_latent, wide_key_weight, preferred_element_type=jnp.float32).astype(jnp.bfloat16).reshape(TOKEN_COUNT, FIRST_HEADS, WIDE_HEAD_SIZE)
    wide_values = jnp.dot(normed_latent, wide_value_weight, preferred_element_type=jnp.float32).astype(jnp.bfloat16).reshape(TOKEN_COUNT, FIRST_HEADS, WIDE_HEAD_SIZE)
    narrow_keys = jnp.dot(normed_latent, narrow_key_weight, preferred_element_type=jnp.float32).astype(jnp.bfloat16).reshape(TOKEN_COUNT, SECOND_HEADS, NARROW_HEAD_SIZE)
    narrow_values = jnp.dot(normed_latent, narrow_value_weight, preferred_element_type=jnp.float32).astype(jnp.bfloat16).reshape(TOKEN_COUNT, SECOND_HEADS, NARROW_HEAD_SIZE)
    wide_mix = attend_group(wide_plain, wide_turned, wide_keys, wide_values, turned_key, (WIDE_HEAD_SIZE + ROPE) ** (-0.5))
    narrow_mix = attend_group(narrow_plain, narrow_turned, narrow_keys, narrow_values, turned_key, (NARROW_HEAD_SIZE + ROPE) ** (-0.5))
    wide_share = FIRST_HEADS * WIDE_HEAD_SIZE // N_TP
    narrow_share = SECOND_HEADS * NARROW_HEAD_SIZE // N_TP
    projected = jnp.zeros((TOKEN_COUNT, D), jnp.float32)
    for member in range(N_TP):
        partial_value = jnp.dot(wide_mix[:, member * wide_share:(member + 1) * wide_share], out_wide[member * wide_share:(member + 1) * wide_share], preferred_element_type=jnp.float32)
        partial_value = partial_value + jnp.dot(narrow_mix[:, member * narrow_share:(member + 1) * narrow_share], out_narrow[member * narrow_share:(member + 1) * narrow_share], preferred_element_type=jnp.float32)
        projected = projected + rounded(partial_value)
    stream = (residual.astype(jnp.float32) + projected).astype(jnp.bfloat16)
    normed = rms_scale(stream.astype(jnp.float32), ffn_gain).astype(jnp.bfloat16)
    shared_share = SHARED_FF // N_TP
    shared = jnp.zeros((TOKEN_COUNT, D), jnp.float32)
    for member in range(N_TP):
        lower = member * shared_share
        upper = lower + shared_share
        gate_part = jnp.dot(normed, shared_gate[:, lower:upper], preferred_element_type=jnp.float32)
        up_part = jnp.dot(normed, shared_up[:, lower:upper], preferred_element_type=jnp.float32)
        active = (jax.nn.silu(gate_part) * up_part).astype(jnp.bfloat16)
        shared = shared + rounded(jnp.dot(active, shared_down[lower:upper], preferred_element_type=jnp.float32))
    devices_all = N_SP * N_TP
    flat_routes = routes.reshape(devices_all, ROWS * TOPK)
    choose = (flat_routes[:, :, None] == jnp.arange(EXPERTS, dtype=jnp.int32)[None, None, :]).astype(jnp.int32)
    earlier = jnp.cumsum(choose, axis=1) - choose
    slots = lax.optimization_barrier(jnp.sum(earlier * choose, axis=2)).astype(jnp.int32)
    device_ids = jnp.broadcast_to(jnp.arange(devices_all, dtype=jnp.int32)[:, None], flat_routes.shape)
    token_of = (device_ids * ROWS + jnp.arange(ROWS * TOPK, dtype=jnp.int32)[None, :] // TOPK).astype(jnp.int32)
    table = jnp.zeros((EXPERTS, devices_all, CAP), jnp.int32).at[flat_routes, device_ids, slots].set(token_of)

    def run_expert(member):
        rows_in = normed[table[member].reshape(-1)]
        gate_part = jnp.dot(rows_in, expert_gate[member], preferred_element_type=jnp.float32)
        up_part = jnp.dot(rows_in, expert_up[member], preferred_element_type=jnp.float32)
        active = (jax.nn.silu(gate_part) * up_part).astype(jnp.bfloat16)
        return jnp.dot(active, expert_down[member], preferred_element_type=jnp.float32).astype(jnp.bfloat16)
    results = lax.map(run_expert, jnp.arange(EXPERTS, dtype=jnp.int32))
    picked = results[flat_routes, device_ids * CAP + slots]
    routed = lax.optimization_barrier(jnp.sum(picked.reshape(TOKEN_COUNT, TOPK, D).astype(jnp.float32) * route_weights[:, :, None], axis=1))
    return (stream.astype(jnp.float32) + shared + routed).astype(jnp.bfloat16)
```

```python
import math

import jax
import jax.numpy as jnp
from jax import lax
from jax.experimental import pallas as pl
from jax.experimental.pallas import tpu as pltpu
from jax.sharding import PartitionSpec as P

ROPE = 64
WIDE_HEAD_SIZE = 128
NARROW_HEAD_SIZE = 64


MESH = pl.DeviceIdType.MESH
VMEM = pl.BlockSpec(memory_space=pltpu.VMEM)


def flip(index, bits):
    mask = 1
    while mask <= bits:
        if bits & mask:
            index = index + mask - 2 * mask * ((index // mask) % 2)
        mask *= 2
    return index


def masks_of(count):
    return [1 << k for k in range(count.bit_length() - 1)]


def low_bit(number):
    return number & -number


def greet(partners):
    barrier = pltpu.get_barrier_semaphore()
    for partner in partners:
        pl.semaphore_signal(barrier, inc=1, device_id=partner, device_id_type=MESH)
    pl.semaphore_wait(barrier, len(partners))


def doubling_order(count):
    return sorted(range(count), key=lambda d: (bin(d).count("1"), -d))


def remote(src, dst, send_sem, recv_sem, target):
    return pltpu.make_async_remote_copy(
        src_ref=src,
        dst_ref=dst,
        send_sem=send_sem,
        recv_sem=recv_sem,
        device_id=target,
        device_id_type=MESH,
    )


def spread_kernel(n_sp, n_tp, x_ref, out_ref, z_send, z_recv, t_send, t_recv, own_sem):
    sp, tp = lax.axis_index("sp"), lax.axis_index("tp")
    tok = x_ref.shape[0]
    part = tok // n_tp
    targets = [{"sp": lax.rem(sp + r, n_sp)} for r in range(1, n_sp)]
    greet(targets + [{"tp": flip(tp, m)} for m in masks_of(n_tp)])

    def rows(block, member):
        return pl.ds(pl.multiple_of(block * tok + member * part, part), part)

    own = pltpu.make_async_copy(
        x_ref, out_ref.at[pl.ds(pl.multiple_of(sp * tok, tok), tok)], own_sem
    )
    sends = []
    for r in range(1, n_sp):
        copy = remote(
            x_ref.at[pl.ds(pl.multiple_of(tp * part, part), part)],
            out_ref.at[rows(sp, tp)],
            z_send.at[r],
            z_recv.at[r],
            targets[r - 1],
        )
        copy.start()
        sends.append(copy)
    own.start()

    def piece(r, d):
        return out_ref.at[rows(lax.rem(sp + n_sp - r, n_sp), flip(tp, d))]

    for d in doubling_order(n_tp):
        for r in range(1, n_sp):
            block = piece(r, d)
            if d == 0:
                sends[r - 1].wait_recv()
            else:
                remote(
                    block, block, t_send.at[r, d], t_recv.at[r, d], {"tp": flip(tp, low_bit(d))}
                ).wait_recv()
            for mask in reversed(masks_of(low_bit(d) if d else n_tp)):
                copy = remote(
                    block,
                    block,
                    t_send.at[r, d + mask],
                    t_recv.at[r, d + mask],
                    {"tp": flip(tp, mask)},
                )
                copy.start()
                sends.append(copy)
    for copy in sends:
        copy.wait_send()
    own.wait()


def spread(x, n_sp, n_tp):
    tok, width = x.shape
    return pl.pallas_call(
        lambda *refs: spread_kernel(n_sp, n_tp, *refs),
        out_shape=jax.ShapeDtypeStruct((n_sp * tok, width), x.dtype),
        in_specs=[VMEM],
        out_specs=VMEM,
        scratch_shapes=[
            pltpu.SemaphoreType.DMA((n_sp,)),
            pltpu.SemaphoreType.DMA((n_sp,)),
            pltpu.SemaphoreType.DMA((n_sp, n_tp)),
            pltpu.SemaphoreType.DMA((n_sp, n_tp)),
            pltpu.SemaphoreType.DMA,
        ],
        compiler_params=pltpu.CompilerParams(collective_id=0, has_side_effects=True),
        cost_estimate=pl.CostEstimate(flops=0, bytes_accessed=30_000_000, transcendentals=0),
    )(x)


def gather_kernel(n_tp, pieces, x_ref, out_ref, send, recv, own_sem):
    tp = lax.axis_index("tp")
    rows, width = x_ref.shape
    part = width // pieces
    greet([{"tp": flip(tp, m)} for m in masks_of(n_tp)])

    def block(d, c):
        start = pl.multiple_of(flip(tp, d) * rows, rows)
        return out_ref.at[pl.ds(start, rows), pl.ds(c * part, part)]

    own = pltpu.make_async_copy(
        x_ref, out_ref.at[pl.ds(pl.multiple_of(tp * rows, rows), rows)], own_sem
    )
    sends = []
    for d in doubling_order(n_tp):
        for c in range(pieces):
            source = x_ref.at[:, pl.ds(c * part, part)] if d == 0 else block(d, c)
            if d:
                remote(
                    source, source, send.at[d, c], recv.at[d, c], {"tp": flip(tp, low_bit(d))}
                ).wait_recv()
            for mask in reversed(masks_of(low_bit(d) if d else n_tp)):
                copy = remote(
                    source,
                    block(d, c),
                    send.at[d + mask, c],
                    recv.at[d + mask, c],
                    {"tp": flip(tp, mask)},
                )
                copy.start()
                sends.append(copy)
        if d == 0:
            own.start()
    for copy in sends:
        copy.wait_send()
    own.wait()


def gather_rows(x, n_tp, pieces=2):
    rows, width = x.shape
    return pl.pallas_call(
        lambda *refs: gather_kernel(n_tp, pieces, *refs),
        out_shape=jax.ShapeDtypeStruct((n_tp * rows, width), x.dtype),
        in_specs=[VMEM],
        out_specs=VMEM,
        scratch_shapes=[
            pltpu.SemaphoreType.DMA((n_tp, pieces)),
            pltpu.SemaphoreType.DMA((n_tp, pieces)),
            pltpu.SemaphoreType.DMA,
        ],
        compiler_params=pltpu.CompilerParams(collective_id=1, has_side_effects=True),
        cost_estimate=pl.CostEstimate(flops=0, bytes_accessed=40_000_000, transcendentals=0),
    )(x)


def scatter_kernel(n_tp, pieces, pairs, *refs):
    lefts, rights = refs[:pairs], refs[pairs : 2 * pairs]
    out_ref, sent, got, send, recv = refs[2 * pairs :]
    tp = lax.axis_index("tp")
    rows, width = out_ref.shape
    part = width // pieces
    greet([{"tp": flip(tp, m)} for m in masks_of(n_tp)])
    copies = {}

    def product(d, c):
        start = pl.multiple_of(flip(tp, d) * rows, rows)
        total = None
        for left, right in zip(lefts, rights):
            term = jnp.dot(
                left[pl.ds(start, rows), :],
                right[:, pl.ds(c * part, part)],
                preferred_element_type=jnp.float32,
            )
            total = term if total is None else total + term
        return total

    def summed(d, c, below):
        total = product(d, c)
        if below > 1:
            total = total.astype(jnp.bfloat16).astype(jnp.float32)
        for mask in masks_of(below):
            copies[d + mask, c].wait_recv()
            total = total + got[d + mask, :, pl.ds(c * part, part)].astype(jnp.float32)
        return total

    def pass_on(mask, c):
        for d in range(mask, n_tp, 2 * mask):
            sent[d, :, pl.ds(c * part, part)] = summed(d, c, mask).astype(jnp.bfloat16)
            copies[d, c] = remote(
                sent.at[d, :, pl.ds(c * part, part)],
                got.at[d, :, pl.ds(c * part, part)],
                send.at[d, c],
                recv.at[d, c],
                {"tp": flip(tp, mask)},
            )
            copies[d, c].start()

    masks = masks_of(n_tp)
    for step in range(pieces + len(masks) - 1):
        for stage, mask in enumerate(masks):
            if 0 <= step - stage < pieces:
                pass_on(mask, step - stage)
    for c in range(pieces):
        out_ref[:, pl.ds(c * part, part)] = summed(0, c, n_tp)
    for copy in copies.values():
        copy.wait_send()


def dot_scatter(lefts, rights, n_tp, collective, pieces=4):
    rows, width = lefts[0].shape[0] // n_tp, rights[0].shape[1]
    pairs = len(lefts)
    return pl.pallas_call(
        lambda *refs: scatter_kernel(n_tp, pieces, pairs, *refs),
        out_shape=jax.ShapeDtypeStruct((rows, width), jnp.float32),
        in_specs=[VMEM] * (2 * pairs),
        out_specs=VMEM,
        scratch_shapes=[
            pltpu.VMEM((n_tp, rows, width), jnp.bfloat16),
            pltpu.VMEM((n_tp, rows, width), jnp.bfloat16),
            pltpu.SemaphoreType.DMA((n_tp, pieces)),
            pltpu.SemaphoreType.DMA((n_tp, pieces)),
        ],
        compiler_params=pltpu.CompilerParams(collective_id=collective, has_side_effects=True),
        cost_estimate=pl.CostEstimate(flops=0, bytes_accessed=40_000_000, transcendentals=0),
    )(*lefts, *rights)


EPS = 1e-06
ROPE_BASE = 10000.0
NEG_FILL = -1e30


def rotate(values, positions):
    half_size = values.shape[-1] // 2
    inverse = ROPE_BASE ** (-jnp.arange(half_size, dtype=jnp.float32) * 2.0 / values.shape[-1])
    angles = positions.astype(jnp.float32)[:, None] * inverse[None, :]
    shaped = (angles.shape[0],) + (1,) * (values.ndim - 2) + (half_size,)
    cosine_table = jnp.cos(angles).reshape(shaped)
    sine_table = jnp.sin(angles).reshape(shaped)
    first_half = values[..., :half_size]
    second_half = values[..., half_size:]
    return jnp.concatenate(
        [
            first_half * cosine_table - second_half * sine_table,
            second_half * cosine_table + first_half * sine_table,
        ],
        axis=-1,
    )


def rms_scale(values, gain):
    return values * lax.rsqrt(jnp.mean(values * values, axis=-1, keepdims=True) + EPS) * gain


def update(state, query_plain, query_turned, keys, turned_rows, values, visible, factor):
    running_max, running_sum, weighted = state
    scores = jnp.einsum("qhd,khd->hqk", query_plain, keys, preferred_element_type=jnp.float32)
    scores = scores + jnp.einsum(
        "qhr,kr->hqk", query_turned, turned_rows, preferred_element_type=jnp.float32
    )
    scores = jnp.where(visible[None], scores * factor, NEG_FILL)
    new_max = jnp.maximum(running_max, jnp.max(scores, axis=2))
    probs = jnp.where(visible[None], jnp.exp(scores - new_max[:, :, None]), 0.0)
    fading = jnp.exp(running_max - new_max)
    running_sum = running_sum * fading + jnp.sum(probs, axis=2)
    weighted = weighted * fading[:, :, None] + jnp.einsum(
        "hqk,khd->hqd", probs.astype(jnp.bfloat16), values, preferred_element_type=jnp.float32
    )
    return (new_max, running_sum, weighted)


def empty_state(heads, queries, value_size):
    return (
        jnp.full((heads, queries), NEG_FILL, jnp.float32),
        jnp.zeros((heads, queries), jnp.float32),
        jnp.zeros((heads, queries, value_size), jnp.float32),
    )


def finish(state):
    normal_sampler = state[2] / state[1][:, :, None]
    heads, queries, value_size = normal_sampler.shape
    return (
        normal_sampler.astype(jnp.bfloat16).transpose(1, 0, 2).reshape(queries, heads * value_size)
    )


def body(
    latent,
    rope_key,
    wide_query,
    narrow_query,
    wide_key_weight,
    wide_value_weight,
    narrow_key_weight,
    narrow_value_weight,
    latent_norm_scale,
    out_wide,
    out_narrow,
    residual,
    ffn_gain,
    shared_gate,
    shared_up,
    shared_down,
    expert_gate,
    expert_up,
    expert_down,
    routes,
    route_weights,
):
    tok_dev = latent.shape[0]
    seq_index = lax.axis_index("sp")
    own_pos = seq_index * tok_dev + jnp.arange(tok_dev, dtype=jnp.int32)
    last_pos = seq_index * tok_dev + tok_dev - 1
    normed_latent = rms_scale(latent.astype(jnp.float32), latent_norm_scale).astype(jnp.bfloat16)
    turned_key = rotate(rope_key.astype(jnp.float32), own_pos).astype(jnp.bfloat16)
    wide_heads_q = wide_query.reshape(tok_dev, -1, WIDE_HEAD_SIZE + ROPE)
    wide_plain = wide_heads_q[..., :WIDE_HEAD_SIZE]
    wide_turned = rotate(wide_heads_q[..., WIDE_HEAD_SIZE:].astype(jnp.float32), own_pos).astype(
        jnp.bfloat16
    )
    narrow_heads_q = narrow_query.reshape(tok_dev, -1, NARROW_HEAD_SIZE + ROPE)
    narrow_plain = narrow_heads_q[..., :NARROW_HEAD_SIZE]
    narrow_turned = rotate(
        narrow_heads_q[..., NARROW_HEAD_SIZE:].astype(jnp.float32), own_pos
    ).astype(jnp.bfloat16)
    wide_local = wide_plain.shape[1]
    narrow_local = narrow_plain.shape[1]
    wide_factor = (WIDE_HEAD_SIZE + ROPE) ** (-0.5)
    narrow_factor = (NARROW_HEAD_SIZE + ROPE) ** (-0.5)
    initial = empty_state(wide_local, tok_dev, WIDE_HEAD_SIZE) + empty_state(
        narrow_local, tok_dev, NARROW_HEAD_SIZE
    )
    n_sp, n_tp = lax.axis_size("sp"), lax.axis_size("tp")
    latent_width = latent.shape[1]
    packed = jnp.concatenate(
        [normed_latent, jnp.pad(turned_key, ((0, 0), (0, -turned_key.shape[1] % 128)))], axis=1
    )
    packed = spread(packed, n_sp, n_tp)
    pieces = (packed[:, :latent_width], packed[:, latent_width : latent_width + ROPE])
    indices = jnp.arange(pieces[0].shape[0], dtype=jnp.int32)
    placing = lambda positions: positions
    latent_rows, turned_rows = pieces
    length_rows = latent_rows.shape[0]
    block = math.gcd(length_rows, 512)

    def one_block(block_index, inner):
        lat_block = lax.dynamic_slice_in_dim(latent_rows, block_index * block, block, 0)
        turned_block = lax.dynamic_slice_in_dim(turned_rows, block_index * block, block, 0)
        key_pos = placing(lax.dynamic_slice_in_dim(indices, block_index * block, block, 0))

        def work(current):
            visible = key_pos[None, :] <= own_pos[:, None]
            wide_keys = (
                jnp.dot(lat_block, wide_key_weight, preferred_element_type=jnp.float32)
                .astype(jnp.bfloat16)
                .reshape(block, wide_local, WIDE_HEAD_SIZE)
            )
            wide_values = (
                jnp.dot(lat_block, wide_value_weight, preferred_element_type=jnp.float32)
                .astype(jnp.bfloat16)
                .reshape(block, wide_local, WIDE_HEAD_SIZE)
            )
            narrow_keys = (
                jnp.dot(lat_block, narrow_key_weight, preferred_element_type=jnp.float32)
                .astype(jnp.bfloat16)
                .reshape(block, narrow_local, NARROW_HEAD_SIZE)
            )
            narrow_values = (
                jnp.dot(lat_block, narrow_value_weight, preferred_element_type=jnp.float32)
                .astype(jnp.bfloat16)
                .reshape(block, narrow_local, NARROW_HEAD_SIZE)
            )
            wide_state = update(
                current[:3],
                wide_plain,
                wide_turned,
                wide_keys,
                turned_block,
                wide_values,
                visible,
                wide_factor,
            )
            narrow_state = update(
                current[3:],
                narrow_plain,
                narrow_turned,
                narrow_keys,
                turned_block,
                narrow_values,
                visible,
                narrow_factor,
            )
            return wide_state + narrow_state

        return lax.cond(jnp.min(key_pos) <= last_pos, work, lambda current: current, inner)

    final = lax.fori_loop(0, length_rows // block, one_block, initial)
    wide_mix = finish(final[:3])
    narrow_mix = finish(final[3:])
    projected = dot_scatter((wide_mix, narrow_mix), (out_wide, out_narrow), n_tp, 2)
    stream = (residual.astype(jnp.float32) + projected).astype(jnp.bfloat16)
    normed = rms_scale(stream.astype(jnp.float32), ffn_gain).astype(jnp.bfloat16)
    piece = gather_rows(normed, n_tp)
    gate_part = jnp.dot(piece, shared_gate, preferred_element_type=jnp.float32)
    up_part = jnp.dot(piece, shared_up, preferred_element_type=jnp.float32)
    active = (jax.nn.silu(gate_part) * up_part).astype(jnp.bfloat16)
    shared = dot_scatter((active,), (shared_down,), n_tp, 3)
    rows_here, top_count = routes.shape
    local_experts = expert_gate.shape[0]
    experts_all = local_experts * lax.axis_size(("sp", "tp"))
    capacity = max(2, 2 * top_count * rows_here // experts_all)
    model_width = normed.shape[1]
    flat_routes = routes.reshape(-1)
    assigned = flat_routes.shape[0]
    choose = (flat_routes[:, None] == jnp.arange(experts_all, dtype=jnp.int32)[None, :]).astype(
        jnp.float32
    )
    lower_mask = (jnp.arange(assigned)[:, None] > jnp.arange(assigned)[None, :]).astype(jnp.float32)
    earlier = jnp.dot(lower_mask, choose, precision=lax.Precision.HIGHEST)
    slots = jnp.sum(earlier * choose, axis=1).astype(jnp.int32)
    target = flat_routes * capacity + slots
    send_map = jnp.any(
        target.reshape(rows_here, top_count)[None, :, :]
        == jnp.arange(experts_all * capacity, dtype=jnp.int32)[:, None, None],
        axis=2,
    ).astype(jnp.bfloat16)
    outgoing = jnp.dot(send_map, normed, preferred_element_type=jnp.float32).astype(jnp.bfloat16)
    outgoing = outgoing.reshape(experts_all, capacity, model_width)
    incoming = lax.all_to_all(outgoing, ("sp", "tp"), split_axis=0, concat_axis=0, tiled=True)
    sources = incoming.shape[0] // local_experts
    grouped = incoming.reshape(sources, local_experts, incoming.shape[1], model_width)
    gate_part = jnp.einsum(
        "sxcd,xdf->sxcf", grouped, expert_gate, preferred_element_type=jnp.float32
    )
    up_part = jnp.einsum("sxcd,xdf->sxcf", grouped, expert_up, preferred_element_type=jnp.float32)
    active = (jax.nn.silu(gate_part) * up_part).astype(jnp.bfloat16)
    finished = jnp.einsum(
        "sxcf,xfd->sxcd", active, expert_down, preferred_element_type=jnp.float32
    ).astype(jnp.bfloat16)
    returned = lax.all_to_all(
        finished.reshape(incoming.shape), ("sp", "tp"), split_axis=0, concat_axis=0, tiled=True
    )
    slot_rows = returned.reshape(experts_all * capacity, model_width)
    by_choice = target.reshape(rows_here, top_count)
    routed = jnp.zeros((rows_here, model_width), jnp.float32)
    for choice in range(top_count):
        hot = by_choice[:, choice : choice + 1] == jnp.arange(experts_all * capacity)[None, :]
        picked = jnp.dot(
            hot.astype(jnp.bfloat16), slot_rows, preferred_element_type=jnp.float32
        )
        routed = routed + picked * route_weights[:, choice : choice + 1]
    return (stream.astype(jnp.float32) + shared + routed).astype(jnp.bfloat16)


def solution(mesh):
    placed = (
        P(("grp", "sp"), None),
        P(("grp", "sp"), None),
        P(("grp", "sp"), "tp"),
        P(("grp", "sp"), "tp"),
        P(None, "tp"),
        P(None, "tp"),
        P(None, "tp"),
        P(None, "tp"),
        P(),
        P("tp", None),
        P("tp", None),
        P(("grp", "sp", "tp"), None),
        P(),
        P(None, "tp"),
        P(None, "tp"),
        P("tp", None),
        P(("sp", "tp"), None, None),
        P(("sp", "tp"), None, None),
        P(("sp", "tp"), None, None),
        P(("grp", "sp", "tp"), None),
        P(("grp", "sp", "tp"), None),
    )
    return jax.shard_map(
        body, mesh=mesh, in_specs=placed, out_specs=P(("grp", "sp", "tp"), None), check_vma=False
    )
```

```python
import jax
import jax.numpy as jnp
from jax import lax
from jax.experimental import pallas as pl
from jax.experimental.pallas import tpu as pltpu
from jax.sharding import PartitionSpec as P

ROPE = 64
WIDE_HEAD_SIZE = 128
NARROW_HEAD_SIZE = 64


MESH = pl.DeviceIdType.MESH
VMEM = pl.BlockSpec(memory_space=pltpu.VMEM)


def flip(index, bits):
    mask = 1
    while mask <= bits:
        if bits & mask:
            index = index + mask - 2 * mask * ((index // mask) % 2)
        mask *= 2
    return index


def masks_of(count):
    return [1 << k for k in range(count.bit_length() - 1)]


def low_bit(number):
    return number & -number


def greet(partners):
    barrier = pltpu.get_barrier_semaphore()
    for partner in partners:
        pl.semaphore_signal(barrier, inc=1, device_id=partner, device_id_type=MESH)
    pl.semaphore_wait(barrier, len(partners))


def doubling_order(count):
    return sorted(range(count), key=lambda d: (bin(d).count("1"), -d))


def remote(src, dst, send_sem, recv_sem, target):
    return pltpu.make_async_remote_copy(
        src_ref=src,
        dst_ref=dst,
        send_sem=send_sem,
        recv_sem=recv_sem,
        device_id=target,
        device_id_type=MESH,
    )


def spread_kernel(n_sp, n_tp, x_ref, out_ref, z_send, z_recv, t_send, t_recv, own_sem):
    sp, tp = lax.axis_index("sp"), lax.axis_index("tp")
    tok = x_ref.shape[0]
    part = tok // n_tp
    targets = [{"sp": lax.rem(sp + r, n_sp)} for r in range(1, n_sp)]
    greet(targets + [{"tp": flip(tp, m)} for m in masks_of(n_tp)])

    def rows(block, member):
        return pl.ds(pl.multiple_of(block * tok + member * part, part), part)

    own = pltpu.make_async_copy(
        x_ref, out_ref.at[pl.ds(pl.multiple_of(sp * tok, tok), tok)], own_sem
    )
    sends = []
    for r in range(1, n_sp):
        copy = remote(
            x_ref.at[pl.ds(pl.multiple_of(tp * part, part), part)],
            out_ref.at[rows(sp, tp)],
            z_send.at[r],
            z_recv.at[r],
            targets[r - 1],
        )
        copy.start()
        sends.append(copy)
    own.start()

    def piece(r, d):
        return out_ref.at[rows(lax.rem(sp + n_sp - r, n_sp), flip(tp, d))]

    for d in doubling_order(n_tp):
        for r in range(1, n_sp):
            block = piece(r, d)
            if d == 0:
                sends[r - 1].wait_recv()
            else:
                remote(
                    block, block, t_send.at[r, d], t_recv.at[r, d], {"tp": flip(tp, low_bit(d))}
                ).wait_recv()
            for mask in reversed(masks_of(low_bit(d) if d else n_tp)):
                copy = remote(
                    block,
                    block,
                    t_send.at[r, d + mask],
                    t_recv.at[r, d + mask],
                    {"tp": flip(tp, mask)},
                )
                copy.start()
                sends.append(copy)
    for copy in sends:
        copy.wait_send()
    own.wait()


def spread(x, n_sp, n_tp):
    tok, width = x.shape
    return pl.pallas_call(
        lambda *refs: spread_kernel(n_sp, n_tp, *refs),
        out_shape=jax.ShapeDtypeStruct((n_sp * tok, width), x.dtype),
        in_specs=[VMEM],
        out_specs=VMEM,
        scratch_shapes=[
            pltpu.SemaphoreType.DMA((n_sp,)),
            pltpu.SemaphoreType.DMA((n_sp,)),
            pltpu.SemaphoreType.DMA((n_sp, n_tp)),
            pltpu.SemaphoreType.DMA((n_sp, n_tp)),
            pltpu.SemaphoreType.DMA,
        ],
        compiler_params=pltpu.CompilerParams(collective_id=0, has_side_effects=True),
        cost_estimate=pl.CostEstimate(flops=0, bytes_accessed=30_000_000, transcendentals=0),
    )(x)


def gather_kernel(
    n_tp, pieces, x_ref, blocks_ref, out_ref, moved_ref, send, recv, own_sem, *semaphores
):
    exchange = Exchange(blocks_ref, moved_ref, *semaphores)
    tp = lax.axis_index("tp")
    rows, width = x_ref.shape
    part = width // pieces
    exchange.greet()

    def block(d, c):
        start = pl.multiple_of(flip(tp, d) * rows, rows)
        return out_ref.at[pl.ds(start, rows), pl.ds(c * part, part)]

    own = pltpu.make_async_copy(
        x_ref, out_ref.at[pl.ds(pl.multiple_of(tp * rows, rows), rows)], own_sem
    )
    sends = []
    for d in doubling_order(n_tp):
        for c in range(pieces):
            source = x_ref.at[:, pl.ds(c * part, part)] if d == 0 else block(d, c)
            if d:
                remote(
                    source, source, send.at[d, c], recv.at[d, c], {"tp": flip(tp, low_bit(d))}
                ).wait_recv()
            for mask in reversed(masks_of(low_bit(d) if d else n_tp)):
                copy = remote(
                    source,
                    block(d, c),
                    send.at[d + mask, c],
                    recv.at[d + mask, c],
                    {"tp": flip(tp, mask)},
                )
                copy.start()
                sends.append(copy)
        if d == 0:
            exchange.start()
            own.start()
    for copy in sends:
        copy.wait_send()
    own.wait()
    exchange.finish()


def gather_rows(x, blocks, n_tp, pieces=2):
    rows, width = x.shape
    return pl.pallas_call(
        lambda *refs: gather_kernel(n_tp, pieces, *refs),
        out_shape=[
            jax.ShapeDtypeStruct((n_tp * rows, width), x.dtype),
            jax.ShapeDtypeStruct(blocks.shape, blocks.dtype),
        ],
        in_specs=[VMEM] * 2,
        out_specs=[VMEM] * 2,
        scratch_shapes=[
            pltpu.SemaphoreType.DMA((n_tp, pieces)),
            pltpu.SemaphoreType.DMA((n_tp, pieces)),
            pltpu.SemaphoreType.DMA,
        ]
        + exchange_semaphores(blocks.shape[0]),
        compiler_params=pltpu.CompilerParams(collective_id=1, has_side_effects=True),
        cost_estimate=pl.CostEstimate(flops=0, bytes_accessed=40_000_000, transcendentals=0),
    )(x, blocks)


def scatter_kernel(n_tp, pieces, pairs, moving, *refs):
    lefts, rights = refs[:pairs], refs[pairs : 2 * pairs]
    refs = refs[2 * pairs :]
    exchange = None
    if moving:
        blocks_ref, out_ref, moved_ref, sent, got, send, recv = refs[:7]
        exchange = Exchange(blocks_ref, moved_ref, *refs[7:])
    else:
        out_ref, sent, got, send, recv = refs
    tp = lax.axis_index("tp")
    rows, width = out_ref.shape
    part = width // pieces
    if moving:
        exchange.greet()
        exchange.start()
    else:
        greet([{"tp": flip(tp, m)} for m in masks_of(n_tp)])
    copies = {}

    def product(d, c):
        start = pl.multiple_of(flip(tp, d) * rows, rows)
        total = None
        for left, right in zip(lefts, rights):
            term = jnp.dot(
                left[pl.ds(start, rows), :],
                right[:, pl.ds(c * part, part)],
                preferred_element_type=jnp.float32,
            )
            total = term if total is None else total + term
        return total

    def summed(d, c, below):
        total = product(d, c)
        if below > 1:
            total = total.astype(jnp.bfloat16).astype(jnp.float32)
        for mask in masks_of(below):
            copies[d + mask, c].wait_recv()
            total = total + got[d + mask, :, pl.ds(c * part, part)].astype(jnp.float32)
        return total

    def pass_on(mask, c):
        for d in range(mask, n_tp, 2 * mask):
            sent[d, :, pl.ds(c * part, part)] = summed(d, c, mask).astype(jnp.bfloat16)
            copies[d, c] = remote(
                sent.at[d, :, pl.ds(c * part, part)],
                got.at[d, :, pl.ds(c * part, part)],
                send.at[d, c],
                recv.at[d, c],
                {"tp": flip(tp, mask)},
            )
            copies[d, c].start()

    masks = masks_of(n_tp)
    for step in range(pieces + len(masks) - 1):
        for stage, mask in enumerate(masks):
            if 0 <= step - stage < pieces:
                pass_on(mask, step - stage)
    for c in range(pieces):
        out_ref[:, pl.ds(c * part, part)] = summed(0, c, n_tp)
    for copy in copies.values():
        copy.wait_send()
    if moving:
        exchange.finish()


def dot_scatter(lefts, rights, n_tp, collective, blocks=None, pieces=4):
    rows, width = lefts[0].shape[0] // n_tp, rights[0].shape[1]
    pairs, moving = len(lefts), blocks is not None
    shapes = [jax.ShapeDtypeStruct((rows, width), jnp.float32)]
    operands = (*lefts, *rights)
    scratch = [
        pltpu.VMEM((n_tp, rows, width), jnp.bfloat16),
        pltpu.VMEM((n_tp, rows, width), jnp.bfloat16),
        pltpu.SemaphoreType.DMA((n_tp, pieces)),
        pltpu.SemaphoreType.DMA((n_tp, pieces)),
    ]
    if moving:
        shapes.append(jax.ShapeDtypeStruct(blocks.shape, blocks.dtype))
        operands += (blocks,)
        scratch += exchange_semaphores(blocks.shape[0])
    return pl.pallas_call(
        lambda *refs: scatter_kernel(n_tp, pieces, pairs, moving, *refs),
        out_shape=shapes,
        in_specs=[VMEM] * len(operands),
        out_specs=[VMEM] * len(shapes),
        scratch_shapes=scratch,
        compiler_params=pltpu.CompilerParams(collective_id=collective, has_side_effects=True),
        cost_estimate=pl.CostEstimate(flops=0, bytes_accessed=40_000_000, transcendentals=0),
    )(*operands)


EPS = 1e-06
ROPE_BASE = 10000.0
NEG_FILL = -1e30


def attend_kernel(sizes, packed, cosine, sine, *refs):
    groups = len(sizes)
    queries, key_ws, value_ws = refs[:groups], refs[groups : 2 * groups], refs[2 * groups : 3 * groups]
    outs = refs[3 * groups : 4 * groups]
    scratch = refs[4 * groups :]
    sp = lax.axis_index("sp")
    tok = cosine.shape[0]
    latent_width = key_ws[0].shape[0]
    lanes = packed.shape[1] - latent_width
    half = ROPE // 2

    def grid(shape):
        return lax.broadcasted_iota(jnp.int32, shape, 0), lax.broadcasted_iota(jnp.int32, shape, 1)

    for g, size in enumerate(sizes):
        plain, turned, peak, total, mixed = scratch[5 * g : 5 * g + 5]
        query = queries[g][...]
        width = query.shape[1]
        for h in range(plain.shape[0]):
            i, j = grid((width, key_ws[g].shape[1]))
            select = (i == j + h * ROPE) & (j >= h * size) & (j < (h + 1) * size)
            plain[h] = jnp.dot(
                query, select.astype(jnp.bfloat16), preferred_element_type=jnp.float32
            ).astype(jnp.bfloat16)
            i, j = grid((width, lanes))
            base = h * (size + ROPE) + size
            same = ((i == j + base) & (j < ROPE)).astype(jnp.float32)
            upper = ((i == j + base + half) & (j < half)).astype(jnp.float32)
            lower = ((i == j + base - half) & (j >= half) & (j < ROPE)).astype(jnp.float32)
            straight = jnp.dot(
                query, same.astype(jnp.bfloat16), preferred_element_type=jnp.float32
            )
            crossed = jnp.dot(
                query, (lower - upper).astype(jnp.bfloat16), preferred_element_type=jnp.float32
            )
            turned[h] = (straight * cosine[...] + crossed * sine[...]).astype(jnp.bfloat16)
        peak[...] = jnp.full_like(peak, NEG_FILL)
        total[...] = jnp.zeros_like(total)
        mixed[...] = jnp.zeros_like(mixed)

    def one_block(index, carry):
        start = pl.ds(pl.multiple_of(index * tok, tok), tok)
        latent = packed[start, :latent_width]
        turned_rows = packed[start, latent_width:]
        i, j = grid((tok, tok))
        visible = index * tok + j <= sp * tok + i
        across = (((1,), (1,)), ((), ()))
        for g, size in enumerate(sizes):
            plain, turned, peak, total, mixed = scratch[5 * g : 5 * g + 5]
            factor = (size + ROPE) ** (-0.5)
            keys = jnp.dot(latent, key_ws[g][...], preferred_element_type=jnp.float32)
            keys = keys.astype(jnp.bfloat16)
            values = jnp.dot(latent, value_ws[g][...], preferred_element_type=jnp.float32)
            values = values.astype(jnp.bfloat16)
            for h in range(plain.shape[0]):
                scores = lax.dot_general(
                    plain[h], keys, across, preferred_element_type=jnp.float32
                ) + lax.dot_general(
                    turned[h], turned_rows, across, preferred_element_type=jnp.float32
                )
                scores = jnp.where(visible, scores * factor, NEG_FILL)
                old = peak[h]
                new = jnp.maximum(old, jnp.max(scores, axis=1, keepdims=True))
                probs = jnp.where(visible, jnp.exp(scores - new), 0.0)
                fading = jnp.exp(old - new)
                peak[h] = new
                total[h] = total[h] * fading + jnp.sum(probs, axis=1, keepdims=True)
                mixed[h] = mixed[h] * fading + jnp.dot(
                    probs.astype(jnp.bfloat16), values, preferred_element_type=jnp.float32
                )
        return carry

    lax.fori_loop(0, sp + 1, one_block, 0)
    for g, size in enumerate(sizes):
        plain, turned, peak, total, mixed = scratch[5 * g : 5 * g + 5]
        i, j = grid(outs[g].shape)
        result = jnp.zeros(outs[g].shape, jnp.float32)
        for h in range(plain.shape[0]):
            own = (j >= h * size) & (j < (h + 1) * size)
            result = jnp.where(own, mixed[h] / total[h], result)
        outs[g][...] = result.astype(jnp.bfloat16)


def attend(packed, cosine, sine, queries, key_ws, value_ws, sizes):
    tok, lanes = cosine.shape
    scratch = []
    for g, size in enumerate(sizes):
        heads = value_ws[g].shape[1] // size
        scratch += [
            pltpu.VMEM((heads, tok, key_ws[g].shape[1]), jnp.bfloat16),
            pltpu.VMEM((heads, tok, lanes), jnp.bfloat16),
            pltpu.VMEM((heads, tok, 1), jnp.float32),
            pltpu.VMEM((heads, tok, 1), jnp.float32),
            pltpu.VMEM((heads, tok, value_ws[g].shape[1]), jnp.float32),
        ]
    return pl.pallas_call(
        lambda *refs: attend_kernel(sizes, *refs),
        out_shape=[jax.ShapeDtypeStruct((tok, w.shape[1]), jnp.bfloat16) for w in value_ws],
        in_specs=[VMEM] * (3 + 3 * len(sizes)),
        out_specs=[VMEM] * len(sizes),
        scratch_shapes=scratch,
    )(packed, cosine, sine, *queries, *key_ws, *value_ws)


class Exchange:
    def __init__(self, source, dest, send, recv, own_sem):
        self.refs = source, dest, send, recv
        self.sp, self.tp = lax.axis_index("sp"), lax.axis_index("tp")
        self.n_sp, self.n_tp = lax.axis_size("sp"), lax.axis_size("tp")
        self.count = self.n_sp * self.n_tp
        self.me = self.sp * self.n_tp + self.tp
        self.own = pltpu.make_async_copy(source.at[self.me], dest.at[self.me], own_sem)

    def target(self, k):
        return (
            lax.rem(self.sp + k // self.n_tp, self.n_sp),
            lax.rem(self.tp + lax.rem(k, self.n_tp), self.n_tp),
        )

    def greet(self):
        barrier = pltpu.get_barrier_semaphore()

        def one(k, carry):
            sp, tp = self.target(k)
            pl.semaphore_signal(
                barrier, inc=1, device_id={"sp": sp, "tp": tp}, device_id_type=MESH
            )
            return carry

        lax.fori_loop(1, self.count, one, 0)
        pl.semaphore_wait(barrier, self.count - 1)

    def copy(self, k):
        source, dest, send, recv = self.refs
        sp, tp = self.target(k)
        return remote(
            source.at[sp * self.n_tp + tp],
            dest.at[self.me],
            send.at[k],
            recv.at[k],
            {"sp": sp, "tp": tp},
        )

    def start(self):
        def one(k, carry):
            self.copy(self.count - k).start()
            return carry

        lax.fori_loop(1, self.count, one, 0)
        self.own.start()

    def finish(self):
        def one(k, carry):
            self.copy(k).wait()
            return carry

        lax.fori_loop(1, self.count, one, 0)
        self.own.wait()


def exchange_semaphores(count):
    return [
        pltpu.SemaphoreType.DMA((count,)),
        pltpu.SemaphoreType.DMA((count,)),
        pltpu.SemaphoreType.DMA,
    ]


def rms_scale(values, gain):
    return values * lax.rsqrt(jnp.mean(values * values, axis=-1, keepdims=True) + EPS) * gain


def body(
    latent,
    rope_key,
    wide_query,
    narrow_query,
    wide_key_weight,
    wide_value_weight,
    narrow_key_weight,
    narrow_value_weight,
    latent_norm_scale,
    out_wide,
    out_narrow,
    residual,
    ffn_gain,
    shared_gate,
    shared_up,
    shared_down,
    expert_gate,
    expert_up,
    expert_down,
    routes,
    route_weights,
):
    tok_dev = latent.shape[0]
    seq_index = lax.axis_index("sp")
    own_pos = seq_index * tok_dev + jnp.arange(tok_dev, dtype=jnp.int32)
    n_sp, n_tp = lax.axis_size("sp"), lax.axis_size("tp")
    normed_latent = rms_scale(latent.astype(jnp.float32), latent_norm_scale).astype(jnp.bfloat16)
    half = ROPE // 2
    lane = jnp.arange(ROPE + -ROPE % 128, dtype=jnp.int32)
    inverse = ROPE_BASE ** (-(lane % half).astype(jnp.float32) * 2.0 / ROPE)
    angles = own_pos.astype(jnp.float32)[:, None] * inverse[None, :]
    cosine, sine = jnp.cos(angles), jnp.sin(angles)
    row = jnp.arange(ROPE, dtype=jnp.int32)[:, None]
    same = (row == lane[None, :]).astype(jnp.bfloat16)
    cross = (row == lane[None, :] - half).astype(jnp.bfloat16) * (lane < ROPE)[None, :] - (
        (row == lane[None, :] + half) & (lane < half)[None, :]
    ).astype(jnp.bfloat16)
    turned_key = (
        jnp.dot(rope_key, same, preferred_element_type=jnp.float32) * cosine
        + jnp.dot(rope_key, cross.astype(jnp.bfloat16), preferred_element_type=jnp.float32) * sine
    ).astype(jnp.bfloat16)
    packed = spread(jnp.concatenate([normed_latent, turned_key], axis=1), n_sp, n_tp)
    wide_mix, narrow_mix = attend(
        packed,
        cosine,
        sine,
        (wide_query, narrow_query),
        (wide_key_weight, narrow_key_weight),
        (wide_value_weight, narrow_value_weight),
        (WIDE_HEAD_SIZE, NARROW_HEAD_SIZE),
    )
    (projected,) = dot_scatter((wide_mix, narrow_mix), (out_wide, out_narrow), n_tp, 2)
    stream = (residual.astype(jnp.float32) + projected).astype(jnp.bfloat16)
    normed = rms_scale(stream.astype(jnp.float32), ffn_gain).astype(jnp.bfloat16)
    rows_here, top_count = routes.shape
    local_experts = expert_gate.shape[0]
    experts_all = local_experts * lax.axis_size(("sp", "tp"))
    capacity = max(2, 2 * top_count * rows_here // experts_all)
    model_width = normed.shape[1]
    flat_routes = routes.reshape(-1)
    assigned = flat_routes.shape[0]
    choose = (flat_routes[:, None] == jnp.arange(experts_all, dtype=jnp.int32)[None, :]).astype(
        jnp.float32
    )
    lower_mask = (jnp.arange(assigned)[:, None] > jnp.arange(assigned)[None, :]).astype(jnp.float32)
    earlier = jnp.dot(lower_mask, choose, precision=lax.Precision.HIGHEST)
    slots = jnp.sum(earlier * choose, axis=1).astype(jnp.int32)
    target = flat_routes * capacity + slots
    send_map = jnp.any(
        target.reshape(rows_here, top_count)[None, :, :]
        == jnp.arange(experts_all * capacity, dtype=jnp.int32)[:, None, None],
        axis=2,
    ).astype(jnp.bfloat16)
    outgoing = jnp.dot(send_map, normed, preferred_element_type=jnp.float32).astype(jnp.bfloat16)
    devices = n_sp * n_tp
    outgoing = outgoing.reshape(devices, local_experts * capacity, model_width)
    piece, incoming = gather_rows(normed, outgoing, n_tp)
    sources = devices
    incoming = incoming.reshape(experts_all, capacity, model_width)
    grouped = incoming.reshape(sources, local_experts, incoming.shape[1], model_width)
    gate_part = jnp.einsum(
        "sxcd,xdf->sxcf", grouped, expert_gate, preferred_element_type=jnp.float32
    )
    up_part = jnp.einsum("sxcd,xdf->sxcf", grouped, expert_up, preferred_element_type=jnp.float32)
    active = (jax.nn.silu(gate_part) * up_part).astype(jnp.bfloat16)
    finished = jnp.einsum(
        "sxcf,xfd->sxcd", active, expert_down, preferred_element_type=jnp.float32
    ).astype(jnp.bfloat16)
    gate_part = jnp.dot(piece, shared_gate, preferred_element_type=jnp.float32)
    up_part = jnp.dot(piece, shared_up, preferred_element_type=jnp.float32)
    active = (jax.nn.silu(gate_part) * up_part).astype(jnp.bfloat16)
    shared, returned = dot_scatter(
        (active,), (shared_down,), n_tp, 3, finished.reshape(outgoing.shape)
    )
    slot_rows = returned.reshape(experts_all * capacity, model_width)
    by_choice = target.reshape(rows_here, top_count)
    routed = jnp.zeros((rows_here, model_width), jnp.float32)
    for choice in range(top_count):
        hot = by_choice[:, choice : choice + 1] == jnp.arange(experts_all * capacity)[None, :]
        picked = jnp.dot(
            hot.astype(jnp.bfloat16), slot_rows, preferred_element_type=jnp.float32
        )
        routed = routed + picked * route_weights[:, choice : choice + 1]
    return (stream.astype(jnp.float32) + shared + routed).astype(jnp.bfloat16)


def solution(mesh):
    placed = (
        P(("grp", "sp"), None),
        P(("grp", "sp"), None),
        P(("grp", "sp"), "tp"),
        P(("grp", "sp"), "tp"),
        P(None, "tp"),
        P(None, "tp"),
        P(None, "tp"),
        P(None, "tp"),
        P(),
        P("tp", None),
        P("tp", None),
        P(("grp", "sp", "tp"), None),
        P(),
        P(None, "tp"),
        P(None, "tp"),
        P("tp", None),
        P(("sp", "tp"), None, None),
        P(("sp", "tp"), None, None),
        P(("sp", "tp"), None, None),
        P(("grp", "sp", "tp"), None),
        P(("grp", "sp", "tp"), None),
    )
    return jax.shard_map(
        body, mesh=mesh, in_specs=placed, out_specs=P(("grp", "sp", "tp"), None), check_vma=False
    )
```
